32 devices in a mesh: sp: 4 (over z), tp: 4 (over y, x), dp: 2 (over core).
Axes of the slice: x: 2, y: 2, z: 4, core: 2. Of those that a mesh axis runs over, the one named last changes fastest.
Arguments:
- latent: bfloat16 [2, 3072, 2048], P('dp', ('sp', 'tp')), may hold values from -3 to 3
- cond: bfloat16 [2, 2048], P('dp', 'sp'), may hold values from -6 to 6
- cond_ctx: bfloat16 [2048], P('sp'), may hold values from -6 to 6
- context: bfloat16 [2, 512, 2048], P('dp', 'sp'), may hold values from -6 to 6
- norm_gain: bfloat16 [2048], replicated, may hold values from 0.099609375 to 1.8984375
- mod_shift: bfloat16 [2048, 2048], P('sp', 'tp'), may hold values from -0.125 to 0.125
- mod_scale: bfloat16 [2048, 2048], P('sp', 'tp'), may hold values from -0.125 to 0.125
- mod_gate: bfloat16 [2048, 2048], P('sp', 'tp'), may hold values from -0.125 to 0.125
- w_query: bfloat16 [2048, 1024], P(None, 'tp'), may hold values from -0.125 to 0.125
- w_key: bfloat16 [2048, 256], P(None, 'tp'), may hold values from -0.125 to 0.125
- w_value: bfloat16 [2048, 256], P(None, 'tp'), may hold values from -0.125 to 0.125
- q_gain: bfloat16 [64], replicated, may hold values from 1 to 5.5
- k_gain: bfloat16 [64], replicated, may hold values from 1 to 5.5
- ctx_lift: float32 [16], P('tp'), may hold values from 1 to 3
- w_out: bfloat16 [1024, 2048], replicated, may hold values from -1.5 to 1.5
Outputs:
- mixed: bfloat16 [2, 3072, 2048], P('dp', ('sp', 'tp'))
The draws below stay inside these ranges and needn't reach their ends.
All inputs are finite; a program needn't handle non-finite values.
Results may differ from the reference program's by a relative error of at most 0.009.
The reference program's roundings to bfloat16 on the way count: a program that leaves them out, or rounds other values in their place, can miss the bound.
Values may be sent and summed in bfloat16 or wider, within the bound.
A program may use at most 64 MiB of HBM per device.

```python
import jax
import jax.numpy as jnp
from jax import lax

D = 2048
HEADS = 16
KV_HEADS = 4
HD = 64
GRID_W = 128
TOK_DEV = 768
CTX = 512
SAMPLES = 2
LAT = 3072
QW = 1024
KVW = 256
N_SP = 4


def draw_gain(key, salt):
    base = jax.random.uniform(jax.random.fold_in(key, salt), (HD,), jnp.float32, 1.0, 1.8)
    return base.astype(jnp.bfloat16)


def draw_q_gain(key, part):
    return draw_gain(key, 1)


def draw_k_gain(key, part):
    return draw_gain(key, 2)


def level_of(rng, shape, shards, low, top_value):
    def one(dim, blocks):
        draws = jax.random.uniform(jax.random.fold_in(jax.random.fold_in(rng, 6), dim), (blocks,), jnp.float32, low / len(shards), top_value / len(shards))
        return jnp.repeat(jnp.exp(draws), shape[dim] // blocks).reshape((-1,) + (1,) * (len(shape) - dim - 1))

    level = one(*shards[0])
    for cut in shards[1:]:
        level = level * one(*cut)
    return level


def bell_draw(key, dims, spread, reach, shards=(), held_as=jnp.bfloat16):
    entries = spread * jax.random.normal(key, dims, jnp.float32)
    if shards:
        entries = entries * level_of(key, dims, shards, -0.22, 0.18)
    return jnp.clip(entries, -reach, reach).astype(held_as)


def setup_inputs(seed: int = 0) -> dict:
    arg_keys = jax.random.split(jax.random.key(seed), 16)
    return {
        "latent": bell_draw(arg_keys[0], (SAMPLES, LAT, D), 0.5, 3.0, ((0, 2), (1, 16))),
        "cond": bell_draw(arg_keys[1], (SAMPLES, D), 1.0, 6.0, ((0, 2), (1, 4))),
        "cond_ctx": bell_draw(arg_keys[2], (D,), 1.0, 6.0, ((0, 4),)),
        "context": bell_draw(arg_keys[3], (SAMPLES, CTX, D), 1.0, 6.0, ((0, 2), (1, 4))),
        "norm_gain": jnp.clip(1.0 + 0.18 * jax.random.normal(arg_keys[4], (D,), jnp.float32), 0.099609375, 1.8984375).astype(jnp.bfloat16),
        "mod_shift": bell_draw(arg_keys[5], (D, D), D ** -0.5, 0.125, ((0, 4), (1, 4))),
        "mod_scale": bell_draw(arg_keys[6], (D, D), D ** -0.5, 0.125, ((0, 4), (1, 4))),
        "mod_gate": bell_draw(arg_keys[7], (D, D), D ** -0.5, 0.125, ((0, 4), (1, 4))),
        "w_query": bell_draw(arg_keys[8], (D, QW), D ** -0.5, 0.125, ((1, 4),)),
        "w_key": bell_draw(arg_keys[9], (D, KVW), D ** -0.5, 0.125, ((1, 4),)),
        "w_value": bell_draw(arg_keys[10], (D, KVW), D ** -0.5, 0.125, ((1, 4),)),
        "q_gain": draw_q_gain(jax.random.fold_in(arg_keys[15], 71), 0),
        "k_gain": draw_k_gain(jax.random.fold_in(arg_keys[15], 71), 0),
        "ctx_lift": jnp.clip(1.0 + 2.0 * jax.random.uniform(arg_keys[13], (HEADS,), jnp.float32) ** level_of(arg_keys[13], (HEADS,), ((0, 4),), -0.2, 0.2), 1.0, 3.0),
        "w_out": bell_draw(arg_keys[14], (QW, D), (QW // 64) ** -0.5, 1.5),
    }


EPS = 1e-06
THETA = 10000.0

def modulate(row_block, gain_vec, shift_rows, scale_rows):
    values = row_block.astype(jnp.float32)
    normed = values * lax.rsqrt(lax.optimization_barrier(jnp.mean(values * values, axis=-1, keepdims=True)) + EPS) * gain_vec.astype(jnp.float32)
    return (normed * (1.0 + scale_rows) + shift_rows).astype(jnp.bfloat16)

def head_norm(raw_proj, gain_vec):
    samples, tokens, width = raw_proj.shape
    pieces = raw_proj.reshape(samples, tokens, width // HD, HD)
    normed = pieces * lax.rsqrt(lax.optimization_barrier(jnp.mean(pieces * pieces, axis=-1, keepdims=True)) + EPS) * gain_vec.astype(jnp.float32)
    return normed.transpose(0, 2, 1, 3)

def rotate(vector, positions):
    pairs_count = vector.shape[-1] // 4
    grid_row = (positions // GRID_W).astype(jnp.float32)
    grid_col = (positions % GRID_W).astype(jnp.float32)
    inverse = THETA ** (-jnp.arange(pairs_count, dtype=jnp.float32) / pairs_count)
    angles = jnp.concatenate([grid_row[:, None] * inverse, grid_col[:, None] * inverse], axis=-1)
    cosine = jnp.cos(angles)
    sine_val = jnp.sin(angles)
    first_half = vector[..., 0::2]
    second_half = vector[..., 1::2]
    turned = jnp.stack([first_half * cosine - second_half * sine_val, first_half * sine_val + second_half * cosine], axis=-1)
    return turned.reshape(vector.shape)

def attend_head(operands):
    query_head, key_head, value_head, ctx_key_head, ctx_value_head, lift_row = operands
    group_size = query_head.shape[0]
    factor = HD ** (-0.5)
    query_blocks = jnp.moveaxis(query_head.reshape(group_size, N_SP, TOK_DEV, HD), 1, 0)

    def one_block(query_block):
        query_wide = query_block.astype(jnp.float32)
        scores = jnp.einsum('gbd,td->gbt', query_wide, key_head.astype(jnp.float32)) * factor
        ctx_scores = jnp.einsum('gbd,td->gbt', query_wide, ctx_key_head.astype(jnp.float32)) * factor + lift_row[:, None, None]
        peak = jnp.maximum(lax.optimization_barrier(jnp.max(scores, axis=-1)), lax.optimization_barrier(jnp.max(ctx_scores, axis=-1)))
        weights = jnp.exp(scores - peak[..., None])
        ctx_weights = jnp.exp(ctx_scores - peak[..., None])
        total = lax.optimization_barrier(jnp.sum(weights, axis=-1)) + lax.optimization_barrier(jnp.sum(ctx_weights, axis=-1))
        weights_low = lax.optimization_barrier(weights.astype(jnp.bfloat16)).astype(jnp.float32)
        ctx_low = lax.optimization_barrier(ctx_weights.astype(jnp.bfloat16)).astype(jnp.float32)
        summed = jnp.einsum('gbt,td->gbd', weights_low, value_head.astype(jnp.float32))
        summed = summed + jnp.einsum('gbt,td->gbd', ctx_low, ctx_value_head.astype(jnp.float32))
        return (summed / total[..., None]).astype(jnp.bfloat16)
    outputs = lax.map(one_block, query_blocks)
    return jnp.moveaxis(outputs, 0, 1).reshape(group_size, N_SP * TOK_DEV, HD)

def reference(latent, cond, cond_ctx, context, norm_gain, mod_shift, mod_scale, mod_gate, w_query, w_key, w_value, q_gain, k_gain, ctx_lift, w_out):
    samples = latent.shape[0]
    tokens = latent.shape[1]
    group_size = HEADS // KV_HEADS
    active = jax.nn.silu(jnp.concatenate([cond, cond_ctx[None, :]], axis=0).astype(jnp.float32)).astype(jnp.bfloat16)
    shift_rows = jnp.dot(active, mod_shift, preferred_element_type=jnp.float32)
    scale_rows = jnp.dot(active, mod_scale, preferred_element_type=jnp.float32)
    gate_rows = jnp.dot(active, mod_gate, preferred_element_type=jnp.float32)
    modulated = modulate(latent, norm_gain, shift_rows[:samples, None, :], scale_rows[:samples, None, :])
    ctx_mod = modulate(context, norm_gain, shift_rows[samples], scale_rows[samples])
    flat = modulated.reshape(-1, D)
    ctx_flat = ctx_mod.reshape(-1, D)
    qraw = jnp.dot(flat, w_query, preferred_element_type=jnp.float32).reshape(samples, tokens, QW)
    kraw = jnp.dot(flat, w_key, preferred_element_type=jnp.float32).reshape(samples, tokens, KVW)
    value_rows = jnp.dot(flat, w_value, preferred_element_type=jnp.float32).astype(jnp.bfloat16)
    kcraw = jnp.dot(ctx_flat, w_key, preferred_element_type=jnp.float32).reshape(samples, CTX, KVW)
    ctx_value_rows = jnp.dot(ctx_flat, w_value, preferred_element_type=jnp.float32).astype(jnp.bfloat16)
    positions = jnp.arange(tokens, dtype=jnp.int32)
    queries = rotate(head_norm(qraw, q_gain), positions).astype(jnp.bfloat16)
    queries = queries.reshape(samples, KV_HEADS, group_size, tokens, HD)
    key_rows = rotate(head_norm(kraw, k_gain), positions).astype(jnp.bfloat16)
    value_heads = value_rows.reshape(samples, tokens, KV_HEADS, HD).transpose(0, 2, 1, 3)
    ctx_keys = head_norm(kcraw, k_gain).astype(jnp.bfloat16)
    ctx_values = ctx_value_rows.reshape(samples, CTX, KV_HEADS, HD).transpose(0, 2, 1, 3)
    lift_table = ctx_lift.astype(jnp.float32).reshape(KV_HEADS, group_size)
    results = []
    for sample_idx in range(samples):
        attended = lax.map(attend_head, (queries[sample_idx], key_rows[sample_idx], value_heads[sample_idx], ctx_keys[sample_idx], ctx_values[sample_idx], lift_table))
        results.append(attended.transpose(2, 0, 1, 3).reshape(tokens, QW))
    head_rows = jnp.stack(results, axis=0)
    projected = jnp.dot(head_rows.reshape(-1, QW), w_out, preferred_element_type=jnp.float32).reshape(samples, tokens, D)
    return (latent.astype(jnp.float32) + gate_rows[:samples, None, :] * projected).astype(jnp.bfloat16)
```

```python
import functools

import jax
import jax.numpy as jnp
import numpy as np
from jax import lax
from jax.experimental import pallas as pl
from jax.experimental.pallas import tpu as pltpu
from jax.sharding import PartitionSpec as P

HD = 64
GRID_W = 128
EPS = 1e-06
THETA = 10000.0
MESH = pl.DeviceIdType.MESH
LOG2E = 1.4426950408889634


def rope_tables(grid_rows):
    n = HD // 4
    inverse = (np.float32(THETA) ** (-np.arange(n, dtype=np.float32) / np.float32(n))).astype(np.float32)

    def table(count, low):
        angles = (np.arange(count, dtype=np.float32)[:, None] * inverse).astype(np.float32)
        zero = np.zeros((count, 2 * n), np.float32)
        sign = np.tile(np.array([-1.0, 1.0], np.float32), n)
        c = np.repeat(np.cos(angles.astype(np.float64)), 2, axis=1).astype(np.float32)
        s = np.repeat(np.sin(angles.astype(np.float64)), 2, axis=1).astype(np.float32) * sign
        parts = ([c, zero], [s, zero]) if low else ([zero, c], [zero, s])
        return [np.tile(np.concatenate(p, axis=1), (1, 2)) for p in parts]

    return np.stack(table(grid_rows, True)), np.stack(table(GRID_W, False))


def kernel(
    n_sp, n_tp, group,
    latent, cond, cond_ctx, norm_gain, q_gain, k_gain, lift, row_tab, col_tab,
    context_h, mshift_h, mscale_h, mgate_h, wq_h, wk_h, wv_h, wout_h,
    out,
    context, mods_w, wq, wk, wv, wkv, wout,
    raw, part, part_in, mods_all, ab, rope, q_all, kv_all, acc, m_st, l_st, o_send, o_all,
    local_sem, lat_send, lat_recv, pa_send, pa_recv, pb_send, pb_recv, kv_send, kv_recv, o_ssem, o_rsem,
):
    rows = latent.shape[0]
    half = rows // 2
    width = latent.shape[1]
    chunk = width // n_tp
    tokens = rows * n_tp
    ctx_rows = context.shape[0]
    sp = lax.axis_index("sp")
    tp = lax.axis_index("tp")
    tx, ty = tp % 2, tp // 2
    peers = (ty * 2 + (1 - tx), (1 - ty) * 2 + tx, (1 - ty) * 2 + (1 - tx))
    sp_order = sorted(range(1, n_sp), key=lambda d: min(d, n_sp - d))

    local = [
        pltpu.make_async_copy(src, dst, local_sem.at[i])
        for i, (src, dst) in enumerate(
            (
                (mshift_h, mods_w.at[0]),
                (mscale_h, mods_w.at[1]),
                (mgate_h, mods_w.at[2]),
                (context_h, context),
                (wk_h, wk),
                (wv_h, wv),
                (wq_h, wq),
                (wout_h, wout),
            )
        )
    ]
    for copy in local:
        copy.start()

    barrier = pltpu.get_barrier_semaphore()
    for peer in peers:
        pl.semaphore_signal(barrier, inc=1, device_id={"tp": peer}, device_id_type=MESH)
    for d in range(1, n_sp):
        pl.semaphore_signal(barrier, inc=1, device_id={"sp": (sp + d) % n_sp}, device_id_type=MESH)
    pl.semaphore_wait(barrier, n_tp - 1 + n_sp - 1)

    def send(src, dst, ssem, rsem, device):
        return pltpu.make_async_remote_copy(
            src_ref=src, dst_ref=dst, send_sem=ssem, recv_sem=rsem, device_id=device, device_id_type=MESH
        )

    top, low = pl.ds(0, half), pl.ds(half, half)
    lat = []

    def send_rows(index, src, slot, piece, peer):
        copy = send(src, raw.at[slot, piece], lat_send.at[index], lat_recv.at[index], {"tp": peer})
        copy.start()
        lat.append(copy)

    send_rows(0, latent.at[top], 0, top, peers[0])
    send_rows(1, latent.at[low], 1, low, peers[1])
    send_rows(2, latent.at[low], 0, low, peers[0])
    send_rows(3, latent.at[top], 1, top, peers[1])

    act = jnp.concatenate([cond[...], cond_ctx[...]], axis=0).astype(jnp.float32)
    act = (act / (1.0 + jnp.exp(-act))).astype(jnp.bfloat16)
    act = jnp.concatenate([act, jnp.zeros((14, act.shape[1]), jnp.bfloat16)], axis=0)
    for i in range(3):
        local[i].wait()
    sums = [jnp.dot(act, mods_w[i], preferred_element_type=jnp.float32)[0:2] for i in range(3)]
    part[...] = jnp.concatenate(sums + [jnp.zeros((2, chunk), jnp.float32)], axis=0)
    pa = []
    for d in sp_order:
        copy = send(part, part_in.at[d - 1], pa_send.at[d - 1], pa_recv.at[d - 1], {"sp": (sp + d) % n_sp})
        copy.start()
        pa.append(copy)

    groups = tokens // GRID_W
    for i in range(2):
        for g in range(groups):
            rope[i, pl.ds(g * GRID_W, GRID_W), :] = (
                row_tab[i, pl.ds(sp * groups + g, 1), :] + col_tab[i, :, :]
            )
    local[4].wait()
    local[5].wait()
    wkv[...] = jnp.concatenate([wk[...], wv[...]], axis=1)

    total = part[...]
    for copy in pa:
        copy.wait_recv()
    for d in range(1, n_sp):
        total = total + part_in[d - 1]
    mods_all[tp] = total
    pb = []
    for i, peer in enumerate(peers):
        copy = send(mods_all.at[tp], mods_all.at[tp], pb_send.at[i], pb_recv.at[i], {"tp": peer})
        copy.start()
        pb.append(copy)
    lat[0].wait_recv()
    send_rows(4, raw.at[0, top], 2, top, peers[1])
    lat[1].wait_recv()
    send_rows(5, raw.at[1, low], 2, low, peers[0])

    for copy in pb:
        copy.wait_recv()
    gain = norm_gain[...].astype(jnp.float32)
    for j in range(n_tp):
        cols = pl.ds(j * chunk, chunk)
        block = mods_all[j]
        ab[0:2, cols] = gain[:, j * chunk : (j + 1) * chunk] * (1.0 + block[2:4])
        ab[2:4, cols] = block[0:2]

    lane = lax.broadcasted_iota(jnp.int32, (1, 2 * HD), 1)
    even = lane % 2 == 0
    left = lane < HD
    ones = (
        (lax.broadcasted_iota(jnp.int32, (2 * HD, 2 * HD), 0) < HD)
        == (lax.broadcasted_iota(jnp.int32, (2 * HD, 2 * HD), 1) < HD)
    ).astype(jnp.bfloat16)
    qg = jnp.concatenate([q_gain[...]] * 2, axis=1).astype(jnp.float32)
    kg = jnp.concatenate([k_gain[...]] * 2, axis=1).astype(jnp.float32)

    def modulated(block, row):
        values = block.astype(jnp.float32)
        scale = lax.rsqrt(jnp.mean(values * values, axis=-1, keepdims=True) + EPS)
        return (values * scale * ab[row : row + 1, :] + ab[row + 2 : row + 3, :]).astype(jnp.bfloat16)

    def headed(x, g):
        square = x * x
        high = square.astype(jnp.bfloat16)
        rest = (square - high.astype(jnp.float32)).astype(jnp.bfloat16)
        mean = (
            jnp.dot(high, ones, preferred_element_type=jnp.float32)
            + jnp.dot(rest, ones, preferred_element_type=jnp.float32)
        ) * (1.0 / HD)
        return x * lax.rsqrt(mean + EPS) * g

    def turned(x, cosine, sine):
        partner = jnp.where(even, pltpu.roll(x, 2 * HD - 1, 1), pltpu.roll(x, 1, 1))
        return x * cosine + partner * sine

    def absorb_rows(block, owner):
        u = modulated(block, 0)
        where = pl.ds(pl.multiple_of(owner * rows, rows), rows)
        cosine, sine = rope[0, where, :], rope[1, where, :]
        kv = jnp.dot(u, wkv[...], preferred_element_type=jnp.float32)
        keys = turned(headed(kv, kg), cosine, sine)
        kv_all[0, where, :] = jnp.where(left, keys, kv).astype(jnp.bfloat16)
        raw_q = jnp.dot(u, wq[...], preferred_element_type=jnp.float32)
        for pair in range(group // 2):
            x = raw_q[:, pair * 2 * HD : (pair + 1) * 2 * HD]
            x = turned(headed(x, qg), cosine, sine)
            q_all[owner * group + 2 * pair] = jnp.where(left, x, 0.0).astype(jnp.bfloat16)
            x = pltpu.roll(x, HD, 1)
            q_all[owner * group + 2 * pair + 1] = jnp.where(left, x, 0.0).astype(jnp.bfloat16)

    local[3].wait()
    uc = modulated(context[...], 1)
    kvc = jnp.dot(uc, wkv[...], preferred_element_type=jnp.float32)
    kv_all[0, pl.ds(tokens, ctx_rows), :] = jnp.where(left, headed(kvc, kg), kvc).astype(jnp.bfloat16)
    local[6].wait()
    absorb_rows(latent[...], tp)
    lat[2].wait_recv()
    absorb_rows(raw[0], peers[0])
    lat[3].wait_recv()
    absorb_rows(raw[1], peers[1])
    lat[4].wait_recv()
    lat[5].wait_recv()
    absorb_rows(raw[2], peers[2])

    kvs = {}
    for d in sp_order:
        copy = send(kv_all.at[0], kv_all.at[d], kv_send.at[d - 1], kv_recv.at[d - 1], {"sp": (sp + d) % n_sp})
        copy.start()
        kvs[d] = copy

    factor = LOG2E * HD ** (-0.5)

    def attend(owner, head, slot, first):
        b = owner * group + head
        kv = kv_all[slot]
        s = lax.dot_general(q_all[b], kv, (((1,), (1,)), ((), ())), preferred_element_type=jnp.float32)
        s_lat = s[:, :tokens]
        s_ctx = s[:, tokens:] + lift[head] * (HD ** 0.5)
        m = jnp.maximum(
            jnp.max(s_lat, axis=1, keepdims=True), jnp.max(s_ctx, axis=1, keepdims=True)
        )
        if not first:
            m_old = m_st[b]
            m = jnp.maximum(m, m_old)
        p_lat = jnp.exp2((s_lat - m) * factor)
        p_ctx = jnp.exp2((s_ctx - m) * factor)
        l = jnp.sum(p_lat, axis=1, keepdims=True) + jnp.sum(p_ctx, axis=1, keepdims=True)
        o = jnp.dot(p_lat.astype(jnp.bfloat16), kv[:tokens], preferred_element_type=jnp.float32)
        o = o + jnp.dot(p_ctx.astype(jnp.bfloat16), kv[tokens:], preferred_element_type=jnp.float32)
        if not first:
            alpha = jnp.exp2((m_old - m) * factor)
            l = l + alpha * l_st[b]
            o = o + alpha * acc[b]
        return b, m, l, o

    order = [0] + sp_order
    for step, slot in enumerate(order[:-1]):
        if step > 0:
            kvs[slot].wait_recv()

        def owner_step(owner, carry, slot=slot, step=step):
            for head in range(group):
                b, m, l, o = attend(owner, head, slot, step == 0)
                m_st[b] = m
                l_st[b] = l
                acc[b] = o
            return carry

        lax.fori_loop(0, n_tp, owner_step, 0)

    slot = order[-1]
    kvs[slot].wait_recv()
    span = group * HD
    mine = pl.ds(pl.multiple_of(tp * span, span), span)
    o_copies = []
    for i, owner in enumerate(peers + (tp,)):
        pieces = []
        for head in range(group):
            b, m, l, o = attend(owner, head, slot, False)
            pieces.append((o / l)[:, HD:].astype(jnp.bfloat16))
        joined = jnp.concatenate(pieces, axis=1)
        if i < n_tp - 1:
            o_send[i] = joined
            copy = send(o_send.at[i], o_all.at[:, mine], o_ssem.at[i], o_rsem.at[i], {"tp": owner})
            copy.start()
            o_copies.append(copy)
        else:
            o_all[:, mine] = joined
    local[7].wait()
    for copy in o_copies:
        copy.wait_recv()

    for j in range(n_tp):
        cols = pl.ds(j * chunk, chunk)
        y = jnp.dot(o_all[...], wout[:, cols], preferred_element_type=jnp.float32)
        gate = mods_all[j, 4:5, :]
        out[:, cols] = (latent[:, cols].astype(jnp.float32) + gate * y).astype(jnp.bfloat16)

    for copy in lat + pa + pb + list(kvs.values()) + o_copies:
        copy.wait_send()


def on_device(n_sp, n_tp, latent, cond, cond_ctx, context, norm_gain, mod_shift, mod_scale, mod_gate,
              w_query, w_key, w_value, q_gain, k_gain, ctx_lift, w_out):
    _, rows, width = latent.shape
    tokens = rows * n_tp
    ctx_rows = context.shape[1]
    group = w_query.shape[1] // w_key.shape[1]
    keys = tokens + ctx_rows
    row_tab, col_tab = rope_tables(tokens * n_sp // GRID_W)
    chunk = mod_shift.shape[1]
    bf, f32 = jnp.bfloat16, jnp.float32
    vmem = pl.BlockSpec(memory_space=pltpu.VMEM)
    smem = pl.BlockSpec(memory_space=pltpu.SMEM)
    hbm = pl.BlockSpec(memory_space=pl.ANY)
    dma = pltpu.SemaphoreType.DMA
    out = pl.pallas_call(
        functools.partial(kernel, n_sp, n_tp, group),
        out_shape=jax.ShapeDtypeStruct((rows, width), bf),
        in_specs=[vmem] * 6 + [smem] + [vmem] * 2 + [hbm] * 8,
        out_specs=vmem,
        scratch_shapes=[
            pltpu.VMEM((ctx_rows, width), bf),
            pltpu.VMEM((3,) + mod_shift.shape, bf),
            pltpu.VMEM(w_query.shape, bf),
            pltpu.VMEM(w_key.shape, bf),
            pltpu.VMEM(w_value.shape, bf),
            pltpu.VMEM((width, 2 * HD), bf),
            pltpu.VMEM(w_out.shape, bf),
            pltpu.VMEM((n_tp - 1, rows, width), bf),
            pltpu.VMEM((8, chunk), f32),
            pltpu.VMEM((n_sp - 1, 8, chunk), f32),
            pltpu.VMEM((n_tp, 8, chunk), f32),
            pltpu.VMEM((8, width), f32),
            pltpu.VMEM((2, tokens, 2 * HD), f32),
            pltpu.VMEM((n_tp * group, rows, 2 * HD), bf),
            pltpu.VMEM((n_sp, keys, 2 * HD), bf),
            pltpu.VMEM((n_tp * group, rows, 2 * HD), f32),
            pltpu.VMEM((n_tp * group, rows, 1), f32),
            pltpu.VMEM((n_tp * group, rows, 1), f32),
            pltpu.VMEM((n_tp - 1, rows, group * HD), bf),
            pltpu.VMEM((rows, n_tp * group * HD), bf),
            dma((8,)),
            dma((6,)), dma((6,)),
            dma((n_sp - 1,)), dma((n_sp - 1,)),
            dma((n_tp - 1,)), dma((n_tp - 1,)),
            dma((n_sp - 1,)), dma((n_sp - 1,)),
            dma((n_tp - 1,)), dma((n_tp - 1,)),
        ],
        compiler_params=pltpu.CompilerParams(
            collective_id=0, has_side_effects=True, vmem_limit_bytes=60 * 1024 * 1024
        ),
    )(
        latent[0], cond, cond_ctx[None], norm_gain[None], q_gain[None], k_gain[None], ctx_lift,
        jnp.asarray(row_tab), jnp.asarray(col_tab),
        context[0], mod_shift, mod_scale, mod_gate, w_query, w_key, w_value, w_out,
    )
    return out[None]


def solution(mesh):
    placed = (
        P("dp", ("sp", "tp"), None),
        P("dp", "sp"),
        P("sp"),
        P("dp", "sp", None),
        P(),
        P("sp", "tp"),
        P("sp", "tp"),
        P("sp", "tp"),
        P(None, "tp"),
        P(None, "tp"),
        P(None, "tp"),
        P(),
        P(),
        P("tp"),
        P(),
    )
    return jax.shard_map(
        functools.partial(on_device, mesh.shape["sp"], mesh.shape["tp"]),
        mesh=mesh,
        in_specs=placed,
        out_specs=P("dp", ("sp", "tp"), None),
        check_vma=False,
    )
```

```python
import functools

import jax
import jax.numpy as jnp
import numpy as np
from jax import lax
from jax.experimental import pallas as pl
from jax.experimental.pallas import tpu as pltpu
from jax.sharding import PartitionSpec as P

HD = 64
GRID_W = 128
EPS = 1e-06
THETA = 10000.0
MESH = pl.DeviceIdType.MESH
LOG2E = 1.4426950408889634
NT = (((1,), (1,)), ((), ()))


def rope_tables(grid_rows):
    n = HD // 4
    inverse = (np.float32(THETA) ** (-np.arange(n, dtype=np.float32) / np.float32(n))).astype(np.float32)

    def table(count, low):
        angles = (np.arange(count, dtype=np.float32)[:, None] * inverse).astype(np.float32)
        zero = np.zeros((count, 2 * n), np.float32)
        sign = np.tile(np.array([-1.0, 1.0], np.float32), n)
        c = np.repeat(np.cos(angles.astype(np.float64)), 2, axis=1).astype(np.float32)
        s = np.repeat(np.sin(angles.astype(np.float64)), 2, axis=1).astype(np.float32) * sign
        parts = ([c, zero], [s, zero]) if low else ([zero, c], [zero, s])
        return [np.tile(np.concatenate(p, axis=1), (1, 2)) for p in parts]

    return np.stack(table(grid_rows, True)), np.stack(table(GRID_W, False))


def kernel(
    n_sp, n_tp, group,
    latent, cond, cond_ctx, norm_gain, q_gain, k_gain, lift, row_tab, col_tab,
    context_h, mshift_h, mscale_h, mgate_h, wq_h, wk_h, wv_h, wout_h,
    out,
    context, mods_w, wq, wkv, wout,
    raw, part, part_in, mods_all, ab, rope, q_all, kv_all, kvt, v_one, lift_col, acc, m_st, o_send, o_all,
    local_sem, lat_send, lat_recv, pa_send, pa_recv, pb_send, pb_recv, kv_send, kv_recv, o_ssem, o_rsem,
):
    rows = latent.shape[0]
    half = rows // 2
    width = latent.shape[1]
    chunk = width // n_tp
    tokens = rows * n_tp
    ctx_rows = context.shape[0]
    sp = lax.axis_index("sp")
    tp = lax.axis_index("tp")
    tx, ty = tp % 2, tp // 2
    peers = (ty * 2 + (1 - tx), (1 - ty) * 2 + tx, (1 - ty) * 2 + (1 - tx))
    sp_order = sorted(range(1, n_sp), key=lambda d: min(d, n_sp - d))

    local = [
        pltpu.make_async_copy(src, dst, local_sem.at[i])
        for i, (src, dst) in enumerate(
            (
                (mshift_h, mods_w.at[0]),
                (mscale_h, mods_w.at[1]),
                (mgate_h, mods_w.at[2]),
                (context_h, context),
                (wk_h, wkv.at[pl.ds(0, HD)]),
                (wv_h, wkv.at[pl.ds(HD, HD)]),
                (wq_h, wq),
                (wout_h, wout),
            )
        )
    ]
    for copy in local:
        copy.start()

    barrier = pltpu.get_barrier_semaphore()
    for peer in peers:
        pl.semaphore_signal(barrier, inc=1, device_id={"tp": peer}, device_id_type=MESH)
    for d in range(1, n_sp):
        pl.semaphore_signal(barrier, inc=1, device_id={"sp": (sp + d) % n_sp}, device_id_type=MESH)
    pl.semaphore_wait(barrier, n_tp - 1 + n_sp - 1)

    def send(src, dst, ssem, rsem, device):
        return pltpu.make_async_remote_copy(
            src_ref=src, dst_ref=dst, send_sem=ssem, recv_sem=rsem, device_id=device, device_id_type=MESH
        )

    top, low = pl.ds(0, half), pl.ds(half, half)
    lat = []

    def send_rows(index, src, slot, piece, peer):
        copy = send(src, raw.at[slot, piece], lat_send.at[index], lat_recv.at[index], {"tp": peer})
        copy.start()
        lat.append(copy)

    send_rows(0, latent.at[top], 0, top, peers[0])
    send_rows(1, latent.at[low], 1, low, peers[1])
    send_rows(2, latent.at[low], 0, low, peers[0])
    send_rows(3, latent.at[top], 1, top, peers[1])

    act = jnp.concatenate([cond[...], cond_ctx[...].reshape(1, -1)], axis=0).astype(jnp.float32)
    act = (act / (1.0 + jnp.exp(-act))).astype(jnp.bfloat16)
    act = jnp.concatenate([act, jnp.zeros((14, act.shape[1]), jnp.bfloat16)], axis=0)
    for i in range(3):
        local[i].wait()
    sums = [jnp.dot(act, mods_w[i], preferred_element_type=jnp.float32)[0:2] for i in range(3)]
    part[...] = jnp.concatenate(sums + [jnp.zeros((2, chunk), jnp.float32)], axis=0)
    pa = []
    for d in sp_order:
        copy = send(part, part_in.at[d - 1], pa_send.at[d - 1], pa_recv.at[d - 1], {"sp": (sp + d) % n_sp})
        copy.start()
        pa.append(copy)

    groups = tokens // GRID_W
    for i in range(2):
        for g in range(groups):
            rope[i, pl.ds(g * GRID_W, GRID_W), :] = (
                row_tab[i, pl.ds(sp * groups + g, 1), :] + col_tab[i, :, :]
            )

    total = part[...]
    for copy in pa:
        copy.wait_recv()
    for d in range(1, n_sp):
        total = total + part_in[d - 1]
    mods_all[tp] = total
    pb = []
    for i, peer in enumerate(peers):
        copy = send(mods_all.at[tp], mods_all.at[tp], pb_send.at[i], pb_recv.at[i], {"tp": peer})
        copy.start()
        pb.append(copy)
    lat[0].wait_recv()
    send_rows(4, raw.at[0, top], 2, top, peers[1])
    lat[1].wait_recv()
    send_rows(5, raw.at[1, low], 2, low, peers[0])

    for copy in pb:
        copy.wait_recv()
    gain = norm_gain[...].astype(jnp.float32).reshape(1, -1)
    for j in range(n_tp):
        cols = pl.ds(j * chunk, chunk)
        block = mods_all[j]
        ab[0:2, cols] = gain[:, j * chunk : (j + 1) * chunk] * (1.0 + block[2:4])
        ab[2:4, cols] = block[0:2]

    lane = lax.broadcasted_iota(jnp.int32, (1, 2 * HD), 1)
    even = lane % 2 == 0
    left = lane < HD
    ones = (
        (lax.broadcasted_iota(jnp.int32, (2 * HD, 2 * HD), 0) < HD)
        == (lax.broadcasted_iota(jnp.int32, (2 * HD, 2 * HD), 1) < HD)
    ).astype(jnp.bfloat16)
    qg = jnp.concatenate([q_gain[...]] * 2, axis=1).astype(jnp.float32)
    kg = jnp.concatenate([k_gain[...]] * 2, axis=1).astype(jnp.float32)

    def modulated(block, row):
        values = block.astype(jnp.float32)
        scale = lax.rsqrt(jnp.mean(values * values, axis=-1, keepdims=True) + EPS)
        return (values * scale * ab[row : row + 1, :] + ab[row + 2 : row + 3, :]).astype(jnp.bfloat16)

    def headed(x, g):
        square = x * x
        high = square.astype(jnp.bfloat16)
        rest = (square - high.astype(jnp.float32)).astype(jnp.bfloat16)
        mean = (
            jnp.dot(high, ones, preferred_element_type=jnp.float32)
            + jnp.dot(rest, ones, preferred_element_type=jnp.float32)
        ) * (1.0 / HD)
        return x * lax.rsqrt(mean + EPS) * g

    def turned(x, cosine, sine):
        partner = jnp.where(even, pltpu.roll(x, 2 * HD - 1, 1), pltpu.roll(x, 1, 1))
        return x * cosine + partner * sine

    def absorb_rows(block, owner):
        u = modulated(block, 0)
        where = pl.ds(pl.multiple_of(owner * rows, rows), rows)
        cosine, sine = rope[0, where, :], rope[1, where, :]
        kv = lax.dot_general(u, wkv[...], NT, preferred_element_type=jnp.float32)
        keys = turned(headed(kv, kg), cosine, sine)
        kv_all[sp, where, :] = jnp.where(left, keys, kv).astype(jnp.bfloat16)
        raw_q = jnp.dot(u, wq[...], preferred_element_type=jnp.float32)
        for pair in range(group // 2):
            x = raw_q[:, pair * 2 * HD : (pair + 1) * 2 * HD]
            x = turned(headed(x, qg), cosine, sine)
            q_all[owner, pl.ds(2 * pair * rows, rows), :] = jnp.where(left, x, 0.0).astype(jnp.bfloat16)
            x = pltpu.roll(x, HD, 1)
            q_all[owner, pl.ds((2 * pair + 1) * rows, rows), :] = jnp.where(left, x, 0.0).astype(jnp.bfloat16)

    local[3].wait()
    local[4].wait()
    local[5].wait()
    uc = modulated(context[...], 1)
    kvc = lax.dot_general(uc, wkv[...], NT, preferred_element_type=jnp.float32)
    kv_all[sp, pl.ds(tokens, ctx_rows), :] = jnp.where(left, headed(kvc, kg), kvc).astype(jnp.bfloat16)
    local[6].wait()
    absorb_rows(latent[...], tp)
    lat[2].wait_recv()
    absorb_rows(raw[0], peers[0])
    lat[3].wait_recv()
    absorb_rows(raw[1], peers[1])
    lat[4].wait_recv()
    lat[5].wait_recv()
    absorb_rows(raw[2], peers[2])

    for head in range(group):
        lift_col[pl.ds(head * rows, rows), :] = jnp.full((rows, 1), lift[head] * (HD ** 0.5), jnp.float32)

    def pass_on(source, side, go):
        copy = send(
            kv_all.at[source], kv_all.at[source], kv_send.at[side, source], kv_recv.at[source],
            {"sp": sp + (1 if side else -1)},
        )
        go(copy)

    def start(copy):
        copy.start()

    def spread(source, side, valid):
        @pl.when(valid & ((sp < n_sp - 1) if side else (sp > 0)))
        def _():
            pass_on(source, side, start)

    spread(sp, 1, sp >= 0)
    spread(sp, 0, sp >= 0)

    factor = LOG2E * HD ** (-0.5)

    def flip(slot):
        kv = kv_all[slot].astype(jnp.float32)
        kvt[...] = kv.T.astype(jnp.bfloat16)
        v_one[...] = jnp.where(left, 1.0, kv).astype(jnp.bfloat16)

    def attend(owner, slot, first):
        s = jnp.dot(q_all[owner], kvt[...], preferred_element_type=jnp.float32)
        s_lat = s[:, :tokens]
        s_ctx = s[:, tokens:] + lift_col[...]
        m = jnp.maximum(
            jnp.max(s_lat, axis=1, keepdims=True), jnp.max(s_ctx, axis=1, keepdims=True)
        )
        if not first:
            m_old = m_st[owner]
            m = jnp.maximum(m, m_old)
        p_lat = jnp.exp2((s_lat - m) * factor)
        p_ctx = jnp.exp2((s_ctx - m) * factor)
        p = jnp.concatenate([p_lat.astype(jnp.bfloat16), p_ctx.astype(jnp.bfloat16)], axis=1)
        o = jnp.dot(p, v_one[...], preferred_element_type=jnp.float32)
        if not first:
            alpha = jnp.exp2((m_old - m) * factor)
            o = o + alpha * acc[owner]
        return m, o

    def keep(owner, slot, first):
        m, o = attend(owner, slot, first)
        m_st[owner] = m
        acc[owner] = o

    after = n_sp - 1 - sp
    near = jnp.minimum(sp, after)
    toward = jnp.where(sp < after, 1, -1)

    def fetch(k):
        both = k <= 2 * near
        distance = jnp.where(both, (k + 1) // 2, k - near)
        way = jnp.where(both & (k % 2 == 0), -toward, toward)

        @pl.when((k > 2 * near) | (k % 2 == 1))
        def _():
            for side in (1, 0):
                source = (sp - distance) if side else (sp + distance)
                inside = (source >= 0) if side else (source <= n_sp - 1)

                @pl.when(inside)
                def _():
                    pass_on(source, side, lambda copy: copy.wait_recv())
                    spread(source, side, inside)

        return sp + way * distance

    flip(sp)
    lax.fori_loop(0, n_tp, lambda owner, c: (keep(owner, sp, True), c)[1], 0)

    def step(k, carry):
        slot = fetch(k)
        flip(slot)
        lax.fori_loop(0, n_tp, lambda owner, c: (keep(owner, slot, False), c)[1], 0)
        return carry

    lax.fori_loop(1, n_sp - 1, step, 0)
    slot = fetch(n_sp - 1)
    flip(slot)
    span = group * HD
    mine = pl.ds(pl.multiple_of(tp * span, span), span)
    o_copies = []
    for i, owner in enumerate(peers + (tp,)):
        m, o = attend(owner, slot, False)
        o = (o / pltpu.roll(o, HD, 1)).astype(jnp.bfloat16)
        joined = jnp.concatenate([o[h * rows : (h + 1) * rows, HD:] for h in range(group)], axis=1)
        if i < n_tp - 1:
            o_send[i] = joined
            copy = send(o_send.at[i], o_all.at[:, mine], o_ssem.at[i], o_rsem.at[i], {"tp": owner})
            copy.start()
            o_copies.append(copy)
        else:
            o_all[:, mine] = joined
    local[7].wait()
    for copy in o_copies:
        copy.wait_recv()

    for j in range(n_tp):
        cols = pl.ds(j * chunk, chunk)
        y = jnp.dot(o_all[...], wout[:, cols], preferred_element_type=jnp.float32)
        gate = mods_all[j, 4:5, :]
        out[:, cols] = (latent[:, cols].astype(jnp.float32) + gate * y).astype(jnp.bfloat16)

    for copy in lat + pa + pb + o_copies:
        copy.wait_send()
    for source in range(n_sp):
        @pl.when((source <= sp) & (sp < n_sp - 1))
        def _():
            pass_on(source, 1, lambda copy: copy.wait_send())

        @pl.when((source >= sp) & (sp > 0))
        def _():
            pass_on(source, 0, lambda copy: copy.wait_send())


def on_device(n_sp, n_tp, latent, cond, cond_ctx, context, norm_gain, mod_shift, mod_scale, mod_gate,
              w_query, w_key, w_value, q_gain, k_gain, ctx_lift, w_out):
    _, rows, width = latent.shape
    tokens = rows * n_tp
    ctx_rows = context.shape[1]
    group = w_query.shape[1] // w_key.shape[1]
    keys = tokens + ctx_rows
    row_tab, col_tab = rope_tables(tokens * n_sp // GRID_W)
    chunk = mod_shift.shape[1]
    bf, f32 = jnp.bfloat16, jnp.float32
    vmem = pl.BlockSpec(memory_space=pltpu.VMEM)
    smem = pl.BlockSpec(memory_space=pltpu.SMEM)
    hbm = pl.BlockSpec(memory_space=pl.ANY)
    dma = pltpu.SemaphoreType.DMA
    out = pl.pallas_call(
        functools.partial(kernel, n_sp, n_tp, group),
        out_shape=jax.ShapeDtypeStruct((rows, width), bf),
        in_specs=[vmem] * 6 + [smem] + [vmem] * 2 + [hbm] * 8,
        out_specs=vmem,
        scratch_shapes=[
            pltpu.VMEM((ctx_rows, width), bf),
            pltpu.VMEM((3,) + mod_shift.shape, bf),
            pltpu.VMEM(w_query.shape, bf),
            pltpu.VMEM((2 * HD, width), bf),
            pltpu.VMEM(w_out.shape, bf),
            pltpu.VMEM((n_tp - 1, rows, width), bf),
            pltpu.VMEM((8, chunk), f32),
            pltpu.VMEM((n_sp - 1, 8, chunk), f32),
            pltpu.VMEM((n_tp, 8, chunk), f32),
            pltpu.VMEM((8, width), f32),
            pltpu.VMEM((2, tokens, 2 * HD), f32),
            pltpu.VMEM((n_tp, group * rows, 2 * HD), bf),
            pltpu.VMEM((n_sp, keys, 2 * HD), bf),
            pltpu.VMEM((2 * HD, keys), bf),
            pltpu.VMEM((keys, 2 * HD), bf),
            pltpu.VMEM((group * rows, 1), f32),
            pltpu.VMEM((n_tp, group * rows, 2 * HD), f32),
            pltpu.VMEM((n_tp, group * rows, 1), f32),
            pltpu.VMEM((n_tp - 1, rows, group * HD), bf),
            pltpu.VMEM((rows, n_tp * group * HD), bf),
            dma((8,)),
            dma((6,)), dma((6,)),
            dma((n_sp - 1,)), dma((n_sp - 1,)),
            dma((n_tp - 1,)), dma((n_tp - 1,)),
            dma((2, n_sp)), dma((n_sp,)),
            dma((n_tp - 1,)), dma((n_tp - 1,)),
        ],
        compiler_params=pltpu.CompilerParams(
            collective_id=0, has_side_effects=True, vmem_limit_bytes=60 * 1024 * 1024
        ),
    )(
        latent[0], cond, cond_ctx, norm_gain, q_gain[None], k_gain[None], ctx_lift,
        jnp.asarray(row_tab), jnp.asarray(col_tab),
        context[0], mod_shift, mod_scale, mod_gate, w_query, w_key.T, w_value.T, w_out,
    )
    return out[None]


def solution(mesh):
    placed = (
        P("dp", ("sp", "tp"), None),
        P("dp", "sp"),
        P("sp"),
        P("dp", "sp", None),
        P(),
        P("sp", "tp"),
        P("sp", "tp"),
        P("sp", "tp"),
        P(None, "tp"),
        P(None, "tp"),
        P(None, "tp"),
        P(),
        P(),
        P("tp"),
        P(),
    )
    return jax.shard_map(
        functools.partial(on_device, mesh.shape["sp"], mesh.shape["tp"]),
        mesh=mesh,
        in_specs=placed,
        out_specs=P("dp", ("sp", "tp"), None),
        check_vma=False,
    )
```

```python
import functools

import jax
import jax.numpy as jnp
import numpy as np
from jax import lax
from jax.experimental import pallas as pl
from jax.experimental.pallas import tpu as pltpu
from jax.sharding import PartitionSpec as P

HD = 64
GRID_W = 128
EPS = 1e-06
THETA = 10000.0
MESH = pl.DeviceIdType.MESH
LOG2E = 1.4426950408889634
NT = (((1,), (1,)), ((), ()))


def rope_tables(grid_rows):
    n = HD // 4
    inverse = (np.float32(THETA) ** (-np.arange(n, dtype=np.float32) / np.float32(n))).astype(np.float32)

    def table(count, low):
        angles = (np.arange(count, dtype=np.float32)[:, None] * inverse).astype(np.float32)
        zero = np.zeros((count, 2 * n), np.float32)
        sign = np.tile(np.array([-1.0, 1.0], np.float32), n)
        c = np.repeat(np.cos(angles.astype(np.float64)), 2, axis=1).astype(np.float32)
        s = np.repeat(np.sin(angles.astype(np.float64)), 2, axis=1).astype(np.float32) * sign
        parts = ([c, zero], [s, zero]) if low else ([zero, c], [zero, s])
        return [np.tile(np.concatenate(p, axis=1), (1, 2)) for p in parts]

    return np.stack(table(grid_rows, True)), np.stack(table(GRID_W, False))


def kernel(
    n_sp, n_tp, group,
    latent, cond, cond_ctx, norm_gain, q_gain, k_gain, lift, row_tab, col_tab,
    context_h, mshift_h, mscale_h, mgate_h, wq_h, wk_h, wv_h, wout_h,
    out,
    context, mods_w, wq, wkv, wout,
    raw, part, part_in, mods_all, ab, rope, q_all, kv_all, kvt, v_one, lift_col, acc, m_st, o_send, o_all,
    local_sem, lat_send, lat_recv, pa_send, pa_recv, pb_send, pb_recv, kv_send, kv_recv, o_ssem, o_rsem,
):
    rows = latent.shape[0]
    half = rows // 2
    width = latent.shape[1]
    chunk = width // n_tp
    tokens = rows * n_tp
    ctx_rows = context.shape[0]
    sp = lax.axis_index("sp")
    tp = lax.axis_index("tp")
    tx, ty = tp % 2, tp // 2
    peers = (ty * 2 + (1 - tx), (1 - ty) * 2 + tx, (1 - ty) * 2 + (1 - tx))
    sp_order = sorted(range(1, n_sp), key=lambda d: min(d, n_sp - d))

    local = [
        pltpu.make_async_copy(src, dst, local_sem.at[i])
        for i, (src, dst) in enumerate(
            (
                (mshift_h, mods_w.at[0]),
                (mscale_h, mods_w.at[1]),
                (mgate_h, mods_w.at[2]),
                (context_h, context),
                (wk_h, wkv.at[pl.ds(0, HD)]),
                (wv_h, wkv.at[pl.ds(HD, HD)]),
                (wq_h, wq),
                (wout_h, wout),
            )
        )
    ]
    for copy in local:
        copy.start()

    barrier = pltpu.get_barrier_semaphore()
    for peer in peers:
        pl.semaphore_signal(barrier, inc=1, device_id={"tp": peer}, device_id_type=MESH)
    for d in range(1, n_sp):
        pl.semaphore_signal(barrier, inc=1, device_id={"sp": (sp + d) % n_sp}, device_id_type=MESH)
    pl.semaphore_wait(barrier, n_tp - 1 + n_sp - 1)

    def send(src, dst, ssem, rsem, device):
        return pltpu.make_async_remote_copy(
            src_ref=src, dst_ref=dst, send_sem=ssem, recv_sem=rsem, device_id=device, device_id_type=MESH
        )

    top, low = pl.ds(0, half), pl.ds(half, half)
    lat = []

    def send_rows(index, src, slot, piece, peer):
        copy = send(src, raw.at[slot, piece], lat_send.at[index], lat_recv.at[index], {"tp": peer})
        copy.start()
        lat.append(copy)

    send_rows(0, latent.at[top], 0, top, peers[0])
    send_rows(1, latent.at[low], 1, low, peers[1])

    act = jnp.concatenate([cond[...], cond_ctx[...].reshape(1, -1)], axis=0).astype(jnp.float32)
    act = (act / (1.0 + jnp.exp(-act))).astype(jnp.bfloat16)
    act = jnp.concatenate([act, jnp.zeros((14, act.shape[1]), jnp.bfloat16)], axis=0)
    for i in range(3):
        local[i].wait()
    sums = [jnp.dot(act, mods_w[i], preferred_element_type=jnp.float32)[0:2] for i in range(3)]
    part[...] = jnp.concatenate(sums + [jnp.zeros((2, chunk), jnp.float32)], axis=0)
    pa = []
    for d in sp_order:
        copy = send(part, part_in.at[d - 1], pa_send.at[d - 1], pa_recv.at[d - 1], {"sp": (sp + d) % n_sp})
        copy.start()
        pa.append(copy)

    groups = tokens // GRID_W
    for i in range(2):
        for g in range(groups):
            rope[i, pl.ds(g * GRID_W, GRID_W), :] = (
                row_tab[i, pl.ds(sp * groups + g, 1), :] + col_tab[i, :, :]
            )

    total = part[...]
    for copy in pa:
        copy.wait_recv()
    for d in range(1, n_sp):
        total = total + part_in[d - 1]
    mods_all[tp] = total
    pb = []
    for i, peer in enumerate(peers):
        copy = send(mods_all.at[tp], mods_all.at[tp], pb_send.at[i], pb_recv.at[i], {"tp": peer})
        copy.start()
        pb.append(copy)
    send_rows(2, latent.at[low], 0, low, peers[0])
    send_rows(3, latent.at[top], 1, top, peers[1])
    lat[0].wait_recv()
    send_rows(4, raw.at[0, top], 2, top, peers[1])
    lat[1].wait_recv()
    send_rows(5, raw.at[1, low], 2, low, peers[0])

    for copy in pb:
        copy.wait_recv()
    gain = norm_gain[...].astype(jnp.float32).reshape(1, -1)
    for j in range(n_tp):
        cols = pl.ds(j * chunk, chunk)
        block = mods_all[j]
        ab[0:2, cols] = gain[:, j * chunk : (j + 1) * chunk] * (1.0 + block[2:4])
        ab[2:4, cols] = block[0:2]

    lane = lax.broadcasted_iota(jnp.int32, (1, 2 * HD), 1)
    even = lane % 2 == 0
    left = lane < HD
    ones = (
        (lax.broadcasted_iota(jnp.int32, (2 * HD, 2 * HD), 0) < HD)
        == (lax.broadcasted_iota(jnp.int32, (2 * HD, 2 * HD), 1) < HD)
    ).astype(jnp.bfloat16)
    qg = jnp.concatenate([q_gain[...]] * 2, axis=1).astype(jnp.float32)
    kg = jnp.concatenate([k_gain[...]] * 2, axis=1).astype(jnp.float32)

    def modulated(block, row):
        values = block.astype(jnp.float32)
        scale = lax.rsqrt(jnp.mean(values * values, axis=-1, keepdims=True) + EPS)
        return (values * scale * ab[row : row + 1, :] + ab[row + 2 : row + 3, :]).astype(jnp.bfloat16)

    def headed(x, g):
        square = x * x
        high = square.astype(jnp.bfloat16)
        rest = (square - high.astype(jnp.float32)).astype(jnp.bfloat16)
        mean = (
            jnp.dot(high, ones, preferred_element_type=jnp.float32)
            + jnp.dot(rest, ones, preferred_element_type=jnp.float32)
        ) * (1.0 / HD)
        return x * lax.rsqrt(mean + EPS) * g

    def turned(x, cosine, sine):
        partner = jnp.where(even, pltpu.roll(x, 2 * HD - 1, 1), pltpu.roll(x, 1, 1))
        return x * cosine + partner * sine

    def absorb_rows(block, owner):
        u = modulated(block, 0)
        where = pl.ds(pl.multiple_of(owner * rows, rows), rows)
        cosine, sine = rope[0, where, :], rope[1, where, :]
        kv = lax.dot_general(u, wkv[...], NT, preferred_element_type=jnp.float32)
        keys = turned(headed(kv, kg), cosine, sine)
        kv_all[sp, where, :] = jnp.where(left, keys, kv).astype(jnp.bfloat16)
        raw_q = jnp.dot(u, wq[...], preferred_element_type=jnp.float32)
        for pair in range(group // 2):
            x = raw_q[:, pair * 2 * HD : (pair + 1) * 2 * HD]
            x = turned(headed(x, qg), cosine, sine)
            q_all[owner, pl.ds(2 * pair * rows, rows), :] = jnp.where(left, x, 0.0).astype(jnp.bfloat16)
            x = pltpu.roll(x, HD, 1)
            q_all[owner, pl.ds((2 * pair + 1) * rows, rows), :] = jnp.where(left, x, 0.0).astype(jnp.bfloat16)

    local[3].wait()
    local[4].wait()
    local[5].wait()
    uc = modulated(context[...], 1)
    kvc = lax.dot_general(uc, wkv[...], NT, preferred_element_type=jnp.float32)
    kv_all[sp, pl.ds(tokens, ctx_rows), :] = jnp.where(left, headed(kvc, kg), kvc).astype(jnp.bfloat16)
    local[6].wait()
    absorb_rows(latent[...], tp)
    lat[2].wait_recv()
    absorb_rows(raw[0], peers[0])
    lat[3].wait_recv()
    absorb_rows(raw[1], peers[1])
    lat[4].wait_recv()
    lat[5].wait_recv()
    absorb_rows(raw[2], peers[2])

    for head in range(group):
        lift_col[pl.ds(head * rows, rows), :] = jnp.full((rows, 1), lift[head] * (HD ** 0.5), jnp.float32)

    def pass_on(source, side, go):
        copy = send(
            kv_all.at[source], kv_all.at[source], kv_send.at[side, source], kv_recv.at[source],
            {"sp": sp + (1 if side else -1)},
        )
        go(copy)

    def start(copy):
        copy.start()

    def spread(source, side, valid):
        @pl.when(valid & ((sp < n_sp - 1) if side else (sp > 0)))
        def _():
            pass_on(source, side, start)

    spread(sp, 1, sp >= 0)
    spread(sp, 0, sp >= 0)

    factor = LOG2E * HD ** (-0.5)

    def flip(slot):
        kv = kv_all[slot].astype(jnp.float32)
        kvt[...] = kv.T.astype(jnp.bfloat16)
        v_one[...] = jnp.where(left, 1.0, kv).astype(jnp.bfloat16)

    def attend(owner, slot, first):
        s = jnp.dot(q_all[owner], kvt[...], preferred_element_type=jnp.float32)
        s_lat = s[:, :tokens]
        s_ctx = s[:, tokens:] + lift_col[...]
        m = jnp.maximum(
            jnp.max(s_lat, axis=1, keepdims=True), jnp.max(s_ctx, axis=1, keepdims=True)
        )
        if not first:
            m_old = m_st[owner]
            m = jnp.maximum(m, m_old)
        p_lat = jnp.exp2((s_lat - m) * factor)
        p_ctx = jnp.exp2((s_ctx - m) * factor)
        p = jnp.concatenate([p_lat.astype(jnp.bfloat16), p_ctx.astype(jnp.bfloat16)], axis=1)
        o = jnp.dot(p, v_one[...], preferred_element_type=jnp.float32)
        if not first:
            alpha = jnp.exp2((m_old - m) * factor)
            o = o + alpha * acc[owner]
        return m, o

    def keep(owner, slot, first):
        m, o = attend(owner, slot, first)
        m_st[owner] = m
        acc[owner] = o

    after = n_sp - 1 - sp
    near = jnp.minimum(sp, after)
    toward = jnp.where(sp < after, 1, -1)

    def fetch(k):
        both = k <= 2 * near
        distance = jnp.where(both, (k + 1) // 2, k - near)
        way = jnp.where(both & (k % 2 == 0), -toward, toward)

        @pl.when((k > 2 * near) | (k % 2 == 1))
        def _():
            for side in (1, 0):
                source = (sp - distance) if side else (sp + distance)
                inside = (source >= 0) if side else (source <= n_sp - 1)

                @pl.when(inside)
                def _():
                    pass_on(source, side, lambda copy: copy.wait_recv())
                    spread(source, side, inside)

        return sp + way * distance

    flip(sp)
    lax.fori_loop(0, n_tp, lambda owner, c: (keep(owner, sp, True), c)[1], 0)

    def step(k, carry):
        slot = fetch(k)
        flip(slot)
        lax.fori_loop(0, n_tp, lambda owner, c: (keep(owner, slot, False), c)[1], 0)
        return carry

    lax.fori_loop(1, n_sp - 1, step, 0)
    slot = fetch(n_sp - 1)
    flip(slot)
    span = group * HD
    mine = pl.ds(pl.multiple_of(tp * span, span), span)
    o_copies = []
    for i, owner in enumerate(peers + (tp,)):
        m, o = attend(owner, slot, False)
        o = (o / pltpu.roll(o, HD, 1)).astype(jnp.bfloat16)
        joined = jnp.concatenate([o[h * rows : (h + 1) * rows, HD:] for h in range(group)], axis=1)
        if i < n_tp - 1:
            o_send[i] = joined
            copy = send(o_send.at[i], o_all.at[:, mine], o_ssem.at[i], o_rsem.at[i], {"tp": owner})
            copy.start()
            o_copies.append(copy)
        else:
            o_all[:, mine] = joined
    local[7].wait()
    for copy in o_copies:
        copy.wait_recv()

    for j in range(n_tp):
        cols = pl.ds(j * chunk, chunk)
        y = jnp.dot(o_all[...], wout[:, cols], preferred_element_type=jnp.float32)
        gate = mods_all[j, 4:5, :]
        out[:, cols] = (latent[:, cols].astype(jnp.float32) + gate * y).astype(jnp.bfloat16)

    for copy in lat + pa + pb + o_copies:
        copy.wait_send()
    for source in range(n_sp):
        @pl.when((source <= sp) & (sp < n_sp - 1))
        def _():
            pass_on(source, 1, lambda copy: copy.wait_send())

        @pl.when((source >= sp) & (sp > 0))
        def _():
            pass_on(source, 0, lambda copy: copy.wait_send())


def on_device(n_sp, n_tp, latent, cond, cond_ctx, context, norm_gain, mod_shift, mod_scale, mod_gate,
              w_query, w_key, w_value, q_gain, k_gain, ctx_lift, w_out):
    _, rows, width = latent.shape
    tokens = rows * n_tp
    ctx_rows = context.shape[1]
    group = w_query.shape[1] // w_key.shape[1]
    keys = tokens + ctx_rows
    row_tab, col_tab = rope_tables(tokens * n_sp // GRID_W)
    chunk = mod_shift.shape[1]
    bf, f32 = jnp.bfloat16, jnp.float32
    vmem = pl.BlockSpec(memory_space=pltpu.VMEM)
    smem = pl.BlockSpec(memory_space=pltpu.SMEM)
    hbm = pl.BlockSpec(memory_space=pl.ANY)
    dma = pltpu.SemaphoreType.DMA
    out = pl.pallas_call(
        functools.partial(kernel, n_sp, n_tp, group),
        out_shape=jax.ShapeDtypeStruct((rows, width), bf),
        in_specs=[vmem] * 6 + [smem] + [vmem] * 2 + [hbm] * 8,
        out_specs=vmem,
        scratch_shapes=[
            pltpu.VMEM((ctx_rows, width), bf),
            pltpu.VMEM((3,) + mod_shift.shape, bf),
            pltpu.VMEM(w_query.shape, bf),
            pltpu.VMEM((2 * HD, width), bf),
            pltpu.VMEM(w_out.shape, bf),
            pltpu.VMEM((n_tp - 1, rows, width), bf),
            pltpu.VMEM((8, chunk), f32),
            pltpu.VMEM((n_sp - 1, 8, chunk), f32),
            pltpu.VMEM((n_tp, 8, chunk), f32),
            pltpu.VMEM((8, width), f32),
            pltpu.VMEM((2, tokens, 2 * HD), f32),
            pltpu.VMEM((n_tp, group * rows, 2 * HD), bf),
            pltpu.VMEM((n_sp, keys, 2 * HD), bf),
            pltpu.VMEM((2 * HD, keys), bf),
            pltpu.VMEM((keys, 2 * HD), bf),
            pltpu.VMEM((group * rows, 1), f32),
            pltpu.VMEM((n_tp, group * rows, 2 * HD), f32),
            pltpu.VMEM((n_tp, group * rows, 1), f32),
            pltpu.VMEM((n_tp - 1, rows, group * HD), bf),
            pltpu.VMEM((rows, n_tp * group * HD), bf),
            dma((8,)),
            dma((6,)), dma((6,)),
            dma((n_sp - 1,)), dma((n_sp - 1,)),
            dma((n_tp - 1,)), dma((n_tp - 1,)),
            dma((2, n_sp)), dma((n_sp,)),
            dma((n_tp - 1,)), dma((n_tp - 1,)),
        ],
        compiler_params=pltpu.CompilerParams(
            collective_id=0, has_side_effects=True, vmem_limit_bytes=60 * 1024 * 1024
        ),
    )(
        latent[0], cond, cond_ctx, norm_gain, q_gain[None], k_gain[None], ctx_lift,
        jnp.asarray(row_tab), jnp.asarray(col_tab),
        context[0], mod_shift, mod_scale, mod_gate, w_query, w_key.T, w_value.T, w_out,
    )
    return out[None]


def solution(mesh):
    placed = (
        P("dp", ("sp", "tp"), None),
        P("dp", "sp"),
        P("sp"),
        P("dp", "sp", None),
        P(),
        P("sp", "tp"),
        P("sp", "tp"),
        P("sp", "tp"),
        P(None, "tp"),
        P(None, "tp"),
        P(None, "tp"),
        P(),
        P(),
        P("tp"),
        P(),
    )
    return jax.shard_map(
        functools.partial(on_device, mesh.shape["sp"], mesh.shape["tp"]),
        mesh=mesh,
        in_specs=placed,
        out_specs=P("dp", ("sp", "tp"), None),
        check_vma=False,
    )
```
